32 devices in a mesh: sp: 8 (over z, x), tp: 4 (over y, core).
Axes of the slice: x: 2, y: 2, z: 4, core: 2. Of those that a mesh axis runs over, the one named last changes fastest.
Arguments:
- residual: bfloat16 [2048, 2048], P(('sp', 'tp')), may hold values from -6 to 6
- queries: bfloat16 [2048, 512], P('sp', 'tp'), may hold values from -6 to 6
- projected_keys: bfloat16 [2048, 512], P('sp', 'tp'), may hold values from -6 to 6
- values: bfloat16 [2048, 1024], P('sp', 'tp'), may hold values from -6 to 6
- projected_output_gate: bfloat16 [2048, 1024], P('sp', 'tp'), may hold values from -6 to 6
- decay_gate_input: bfloat16 [2048, 512], P('sp', 'tp'), may hold values from -7 to 7
- decay_gate_offset: float32 [512], P('tp')
- decay_spikes: float32 [2048, 16], P('sp', 'tp'), may hold values from -3 to 0, as said below
- documents: int32 [2048], P('sp'), may hold values from 0 to 3, as said below
- attention_output_weight: bfloat16 [1024, 2048], P('tp'), may hold values from -0.1875 to 0.1875
- layer_norm_gains: float32 [2, 2048], replicated, may hold values from 0.1 to 1.9
- layer_norm_shifts: float32 [2, 2048], replicated, may hold values from -3 to 3
- routes: int32 [2048, 2], P('sp'), may hold values from 0 to 7, all different within a row; in each aligned block of 64 rows (0 to 63, 64 to 127, ...) at most 32 rows name the same one
- chosen_expert_weights: float32 [2048, 2], P('sp'), may hold values from 0.2 to 1
- expert_gate_weight: bfloat16 [8, 2048, 3584], P('sp', None, 'tp'), may hold values from -0.125 to 0.125
- expert_up_weight: bfloat16 [8, 2048, 3584], P('sp', None, 'tp'), may hold values from -0.125 to 0.125
- expert_down_weight: bfloat16 [8, 3584, 2048], P('sp', 'tp'), may hold values from -0.09375 to 0.09375
Outputs:
- layer_out: bfloat16 [2048, 2048], P(('sp', 'tp'))
The draws below stay inside these ranges and needn't reach their ends.
Inputs may be any that keep to these rules, and one draw needn't show every extreme that they name: `routes`: each row names 2 different experts; in each aligned block of 64 rows no expert is named by more than 32 rows. `documents`: the first position has document 0; document numbers never fall and rise by at most one from a position to the next. `decay_spikes`: zero at all but a few positions.
All inputs are finite; a program needn't handle non-finite values.
Results may differ from the reference program's by a relative error of at most 0.015.
Values may be sent and summed in bfloat16 or wider, within the bound.
No kernel may reach another device: no remote copies, remote signals or barrier semaphores. Data moves between devices by JAX's collectives and lax.ppermute only.
A program may use at most 64 MiB of HBM per device.

```python
import math
import jax
import jax.numpy as jnp
import numpy as np
from jax import lax

D = 2048
FILTERED_MIXERS = 16
DK = 32
DV = 64
FF = 3584
TOPK = 2
BLOCK = 64
SLICE_SPAN = 256
TEXT_POSITIONS = 2048
ROWS_DEV = 64
EXPERTS = 8
CAP = 32
N_TP = 4


def draw_decay_gate_input(key, part):
    noise_key, shift_key = jax.random.split(key)
    noise = jnp.clip(jax.random.normal(noise_key, (TEXT_POSITIONS, FILTERED_MIXERS * DK), jnp.float32), -6.0, 6.0)
    shifts = jax.random.uniform(shift_key, (TEXT_POSITIONS // SLICE_SPAN, FILTERED_MIXERS), jnp.float32, -0.7, 0.7)
    shifts = jnp.repeat(jnp.repeat(shifts, SLICE_SPAN, axis=0), DK, axis=1)
    return (noise + shifts).astype(jnp.bfloat16)


def draw_decay_gate_offset(key, part):
    pick_key, slow_key, fast_key, jitter_key = jax.random.split(key, 4)
    ranks = jax.random.permutation(pick_key, FILTERED_MIXERS)
    slow_heads = ranks < FILTERED_MIXERS // 2
    slow_level = math.log(TEXT_POSITIONS / 4.0) + jax.random.uniform(slow_key, (FILTERED_MIXERS,), jnp.float32, 0.0, 1.5)
    fast_level = jax.random.uniform(fast_key, (FILTERED_MIXERS,), jnp.float32, 0.5, 2.0)
    levels = jnp.where(slow_heads, slow_level, fast_level)
    jitter = jax.random.uniform(jitter_key, (FILTERED_MIXERS, DK), jnp.float32, -0.5, 0.5)
    return (levels[:, None] + jitter).reshape(FILTERED_MIXERS * DK).astype(jnp.float32)


def draw_decay_spikes(key, part):
    placement_seed_handle, strata_seed_handle = jax.random.split(key)
    spike_count_sum = max(2, TEXT_POSITIONS // SLICE_SPAN // 8)
    placement_catalog = jax.random.randint(placement_seed_handle, (spike_count_sum,), 0, TEXT_POSITIONS)
    strata_amounts = jnp.log(jax.random.uniform(strata_seed_handle, (spike_count_sum, FILTERED_MIXERS), jnp.float32, 0.5, 0.8))
    marks = (jnp.arange(TEXT_POSITIONS)[:, None] == placement_catalog[None, :]).astype(jnp.float32)
    return jnp.dot(marks, strata_amounts, precision=lax.Precision.HIGHEST).astype(jnp.float32)


def draw_documents(key, part):
    anchor_key, place_key = jax.random.split(key)
    groups = TEXT_POSITIONS // SLICE_SPAN
    anchor = jax.random.randint(anchor_key, (), 0, groups // 2 - 1)
    device_ids = jnp.arange(groups)
    offset = device_ids - anchor
    has_cut = jnp.where((offset >= 1) & (offset <= groups // 2 + 1), 0, 1).astype(jnp.int32)
    placement_catalog = jax.random.randint(place_key, (groups,), 1, SLICE_SPAN)
    starts = jnp.zeros((TEXT_POSITIONS,), jnp.int32).at[device_ids * SLICE_SPAN + placement_catalog].set(has_cut)
    return jnp.cumsum(starts).astype(jnp.int32)


def steps_of(stream_key, shape, cuts, smallest, largest):
    factor_of = 1.0
    for dim, parts in cuts:
        steps = jax.random.uniform(jax.random.fold_in(jax.random.fold_in(stream_key, 6), dim), (parts,), jnp.float32, smallest / len(cuts), largest / len(cuts))
        factor_of = factor_of * jnp.repeat(jnp.exp(steps), shape[dim] // parts).reshape((-1,) + (1,) * (len(shape) - 1 - dim))
    return factor_of


def assign_block(stream_key, own, number, rows, amount, top, most, skew):
    sequence = jax.random.permutation(stream_key, amount)
    crowded, usual = load_shares(amount, rows * top, most, skew, True), load_shares(amount, rows * top, most, skew, False)
    places = jnp.arange(amount)

    def named(sizes, turn):
        used = int((sizes > 0).sum())
        fixed = max(1, used // 4)
        moved = fixed + (places - fixed + turn * (used - fixed)) % max(1, amount - fixed)
        return jnp.zeros((amount,), jnp.int32).at[sequence[jnp.where(places < fixed, places, moved)]].set(jnp.asarray(sizes, jnp.int32))

    sizes = jnp.where(number % 4 == 0, named(crowded, number // 4), named(usual, number - number // 4 - 1))
    mixed = jax.random.permutation(jax.random.fold_in(own, 3), amount)
    giver, receiver = mixed[0:amount // 2 * 2:2], mixed[1:amount // 2 * 2:2]
    margin = jnp.minimum(sizes[giver] - 1, most - sizes[receiver]) // 2
    margin = jnp.where((giver == sequence[0]) | (receiver == sequence[0]) | (sizes[receiver] == 0), 0, jnp.maximum(margin, 0))
    moved = jax.random.randint(jax.random.fold_in(own, 4), (amount // 2,), 0, 1 << 20) % (margin + 1)
    sizes = sizes.at[giver].add(-moved).at[receiver].add(moved)
    labels = jnp.searchsorted(jnp.cumsum(sizes), jnp.arange(rows * top), side="right").astype(jnp.int32)
    table = labels.reshape(top, rows).T
    table = table[jax.random.permutation(jax.random.fold_in(own, 1), rows)]
    turn = jax.random.randint(jax.random.fold_in(own, 2), (rows, 1), 0, top)
    return jnp.take_along_axis(table, (jnp.arange(top)[None, :] + turn) % top, axis=1)


def load_shares(count, total, reach, lean, full):
    portions = [(1 << 20) // math.isqrt(standing ** lean) + 1 for standing in range(1, count + 1)]
    largest = reach if full else min(reach, max(-(-total // count), total * portions[0] // sum(portions)))
    least = 1 if total - largest >= count - 1 else 0
    holding, rest = [largest] + [least] * (count - 1), total - largest - least * (count - 1)
    while rest > 0:
        candidates = [i for i in range(1, count) if holding[i] < largest] or [i for i in range(1, count) if holding[i] < reach]
        mass, budget = sum([portions[i] for i in candidates]), rest
        for i in candidates:
            more = min(reach - holding[i], max(1, budget * portions[i] // mass), rest)
            holding[i] = holding[i] + more
            rest = rest - more
    return np.array(holding)


def centred(rng, extent, deviation, limit, pieces=(), held_as=jnp.bfloat16):
    level = steps_of(rng, extent, pieces, -0.22, 0.18) if pieces else 1.0
    drawn = jax.random.normal(rng, extent, jnp.float32) * deviation * level
    return jnp.minimum(jnp.maximum(drawn, -limit), limit).astype(held_as)


def setup_inputs(seed: int = 0) -> dict:
    key_of = jax.random.split(jax.random.key(seed), 18)
    residual = centred(key_of[0], (TEXT_POSITIONS, D), 1.0, 6.0, ((0, 32),))
    queries = centred(key_of[1], (TEXT_POSITIONS, FILTERED_MIXERS * DK), 1.0, 6.0, ((0, 8), (1, 4)))
    projected_keys = centred(key_of[2], (TEXT_POSITIONS, FILTERED_MIXERS * DK), 1.0, 6.0, ((0, 8), (1, 4)))
    values = centred(key_of[3], (TEXT_POSITIONS, FILTERED_MIXERS * DV), 1.0, 6.0, ((0, 8), (1, 4)))
    projected_output_gate = centred(key_of[4], (TEXT_POSITIONS, FILTERED_MIXERS * DV), 1.0, 6.0, ((0, 8), (1, 4)))
    decay_gate_input = draw_decay_gate_input(jax.random.fold_in(key_of[17], 71), 0)
    decay_gate_offset = draw_decay_gate_offset(jax.random.fold_in(key_of[17], 71), 0)
    decay_spikes = draw_decay_spikes(jax.random.fold_in(key_of[17], 71), 0)
    documents = draw_documents(jax.random.fold_in(key_of[17], 71), 0)
    attention_output_weight = centred(key_of[9], (FILTERED_MIXERS * DV, D), (FILTERED_MIXERS * DV) ** -0.5, 0.1875, ((0, 4),))
    layer_norm_gains = jnp.clip(1.0 + 0.18 * jax.random.normal(key_of[10], (2, D), jnp.float32), 0.1, 1.9)
    layer_norm_shifts = centred(key_of[11], (2, D), 0.3, 3.0, (), jnp.float32)
    routes_keys = jax.random.split(jax.random.fold_in(key_of[12], 1), TEXT_POSITIONS // ROWS_DEV)
    routes_turns = jax.random.permutation(jax.random.fold_in(key_of[12], 3), TEXT_POSITIONS // ROWS_DEV)
    routes = jax.vmap(lambda own, number: assign_block(jax.random.fold_in(key_of[12], 2), own, number, ROWS_DEV, EXPERTS, TOPK, CAP, 2))(routes_keys, routes_turns).reshape((TEXT_POSITIONS, TOPK))
    chosen_expert_weights = jnp.clip(0.2 + 0.8 * jax.random.uniform(key_of[13], (TEXT_POSITIONS, TOPK), jnp.float32) ** steps_of(key_of[13], (TEXT_POSITIONS, TOPK), ((0, 8),), -0.2, 0.2), 0.2, 1.0)
    expert_gate_weight = centred(key_of[14], (EXPERTS, D, FF), D ** -0.5, 0.125, ((0, 8), (2, 4)))
    expert_up_weight = centred(key_of[15], (EXPERTS, D, FF), D ** -0.5, 0.125, ((0, 8), (2, 4)))
    expert_down_weight = centred(key_of[16], (EXPERTS, FF, D), FF ** -0.5, 0.09375, ((0, 8), (1, 4)))
    return dict(residual=residual, queries=queries, projected_keys=projected_keys, values=values, projected_output_gate=projected_output_gate, decay_gate_input=decay_gate_input, decay_gate_offset=decay_gate_offset, decay_spikes=decay_spikes, documents=documents, attention_output_weight=attention_output_weight, layer_norm_gains=layer_norm_gains, layer_norm_shifts=layer_norm_shifts, routes=routes, chosen_expert_weights=chosen_expert_weights, expert_gate_weight=expert_gate_weight, expert_up_weight=expert_up_weight, expert_down_weight=expert_down_weight)


eps_rms = 1e-06
eps_layer = 1e-05
decay_norm = 16.0
tile_rows = 128

def log_decay_values(decay_gate_input, decay_gate_offset, decay_spikes):
    head_number = decay_spikes.shape[1]
    log_rate_values = jax.nn.log_sigmoid(decay_gate_input.astype(jnp.float32) + decay_gate_offset) / decay_norm
    return log_rate_values.reshape(log_rate_values.shape[0], head_number, -1) + decay_spikes[:, :, None]

def block_pass(carry_in, block_inputs):
    current_state, state_doc = carry_in
    query_block, key_blk, value_block, rate_blk, doc_blk = block_inputs
    sequence_length = doc_blk.shape[0]
    running_total = jnp.cumsum(rate_blk, axis=0)
    row_ids = lax.broadcasted_iota(jnp.int32, (sequence_length, sequence_length), 0)
    col_ids = lax.broadcasted_iota(jnp.int32, (sequence_length, sequence_length), 1)
    visible = (row_ids >= col_ids) & (doc_blk[:, None] == doc_blk[None, :])
    spread = running_total[:, None] - running_total[None, :]
    decay_pairs = jnp.exp(jnp.where(visible[:, :, None, None], spread, -jnp.inf))
    scores = lax.optimization_barrier(jnp.sum(query_block[:, None] * decay_pairs * key_blk[None, :], axis=-1))
    inner_term = jnp.einsum('tsh,shv->thv', scores, value_block)
    active_mask = (doc_blk == state_doc).astype(jnp.float32)
    carried_over = jnp.einsum('nws,wse->nwe', query_block * jnp.exp(running_total), current_state) * active_mask[:, None, None]
    last_doc = doc_blk[sequence_length - 1].astype(jnp.float32)
    tail_mask = (doc_blk == last_doc).astype(jnp.float32)
    document_key_ends = key_blk * jnp.exp(running_total[sequence_length - 1][None] - running_total) * tail_mask[:, None, None]
    keep_state = (state_doc == last_doc).astype(jnp.float32)
    updated_state = current_state * (jnp.exp(running_total[sequence_length - 1]) * keep_state)[:, :, None]
    updated_state = updated_state + jnp.einsum('elr,elo->lro', document_key_ends, value_block)
    return ((updated_state, last_doc), inner_term + carried_over)

def layer_norm(stream, gain_row, shift_row):
    center = lax.optimization_barrier(jnp.mean(stream, axis=-1, keepdims=True))
    spread = lax.optimization_barrier(jnp.mean(jnp.square(stream - center), axis=-1, keepdims=True))
    return (stream - center) * lax.rsqrt(spread + eps_layer) * gain_row + shift_row

def expert_rows(row_block, gate_one, up_one, down_one):
    gate_val = jnp.dot(row_block, gate_one, preferred_element_type=jnp.float32)
    up_val = jnp.dot(row_block, up_one, preferred_element_type=jnp.float32)
    hidden = (jax.nn.silu(gate_val) * up_val).astype(jnp.bfloat16)
    quarter = hidden.shape[1] // N_TP
    summed = jnp.zeros((row_block.shape[0], down_one.shape[1]), jnp.float32)
    for part_index in range(N_TP):
        down_part = jnp.dot(hidden[:, part_index * quarter:(part_index + 1) * quarter], down_one[part_index * quarter:(part_index + 1) * quarter], preferred_element_type=jnp.float32)
        rounded = lax.optimization_barrier(down_part.astype(jnp.bfloat16))
        summed = summed + rounded.astype(jnp.float32)
    return summed

def routed_experts(normed, routes, chosen_expert_weights, expert_gate_weight, expert_up_weight, expert_down_weight):
    top_count = routes.shape[1]
    assign_total = routes.shape[0] * top_count
    expert_count = expert_gate_weight.shape[0]
    assign_expert = routes.reshape(-1).astype(jnp.int32)
    assign_token = (jnp.arange(assign_total, dtype=jnp.int32) // top_count).astype(jnp.int32)
    assign_weight = chosen_expert_weights.reshape(-1)
    sort_order = jnp.argsort(assign_expert, stable=True)
    sorted_expert = assign_expert[sort_order]
    counts = lax.optimization_barrier(jnp.sum((assign_expert[:, None] == jnp.arange(expert_count, dtype=jnp.int32)[None, :]).astype(jnp.int32), axis=0))
    padded = ((counts + tile_rows - 1) // tile_rows * tile_rows).astype(jnp.int32)
    starts = (jnp.cumsum(counts) - counts).astype(jnp.int32)
    pad_end = jnp.cumsum(padded).astype(jnp.int32)
    pad_start = (pad_end - padded).astype(jnp.int32)
    ranks = jnp.arange(assign_total, dtype=jnp.int32)
    dest_rows = (pad_start[sorted_expert] + ranks - starts[sorted_expert]).astype(jnp.int32)
    tile_count = -(-assign_total // tile_rows) + expert_count
    row_token = jnp.zeros((tile_count * tile_rows,), jnp.int32).at[dest_rows].set(assign_token[sort_order])
    row_weight = jnp.zeros((tile_count * tile_rows,), jnp.float32).at[dest_rows].set(assign_weight[sort_order])
    tile_start = jnp.arange(tile_count, dtype=jnp.int32) * tile_rows
    tile_expert = jnp.minimum(lax.optimization_barrier(jnp.sum((tile_start[:, None] >= pad_end[None, :]).astype(jnp.int32), axis=1)), expert_count - 1).astype(jnp.int32)

    def tile_work(tile_inputs):
        token_ids, expert_id = tile_inputs
        return expert_rows(normed[token_ids], expert_gate_weight[expert_id], expert_up_weight[expert_id], expert_down_weight[expert_id])
    tile_out = lax.map(tile_work, (row_token.reshape(tile_count, tile_rows), tile_expert))
    weighted = tile_out.reshape(-1, normed.shape[1]) * row_weight[:, None]
    return jnp.zeros(normed.shape, jnp.float32).at[row_token].add(weighted)

def reference(residual, queries, projected_keys, values, projected_output_gate, decay_gate_input, decay_gate_offset, decay_spikes, documents, attention_output_weight, layer_norm_gains, layer_norm_shifts, routes, chosen_expert_weights, expert_gate_weight, expert_up_weight, expert_down_weight):
    overall_rows, head_number = decay_spikes.shape
    key_dim = queries.shape[1] // head_number
    value_dim = values.shape[1] // head_number
    query_f = queries.astype(jnp.float32).reshape(overall_rows, head_number, key_dim) * key_dim ** (-0.5)
    key_f = projected_keys.astype(jnp.float32).reshape(overall_rows, head_number, key_dim)
    value_float = values.astype(jnp.float32).reshape(overall_rows, head_number, value_dim)
    log_rate_values = log_decay_values(decay_gate_input, decay_gate_offset, decay_spikes)
    block_count = overall_rows // BLOCK

    def blocked(whole_array):
        return whole_array.reshape((block_count, BLOCK) + whole_array.shape[1:])
    start_carry = (jnp.zeros((head_number, key_dim, value_dim), jnp.float32), jnp.array(-1.0, jnp.float32))
    _, block_outputs = lax.scan(block_pass, start_carry, (blocked(query_f), blocked(key_f), blocked(value_float), blocked(log_rate_values), blocked(documents)))
    recurrent = block_outputs.reshape(overall_rows, head_number, value_dim)
    norm_scale = lax.rsqrt(lax.optimization_barrier(jnp.mean(recurrent * recurrent, axis=-1, keepdims=True)) + eps_rms)
    gate_act = jax.nn.silu(projected_output_gate.astype(jnp.float32).reshape(overall_rows, head_number, value_dim))
    mixed = (recurrent * norm_scale * gate_act).reshape(overall_rows, head_number * value_dim).astype(jnp.bfloat16)
    projected = jnp.dot(mixed, attention_output_weight, preferred_element_type=jnp.float32)
    normed = layer_norm(residual.astype(jnp.float32) + projected, layer_norm_gains[0], layer_norm_shifts[0]).astype(jnp.bfloat16)
    expert_mix = routed_experts(normed, routes, chosen_expert_weights, expert_gate_weight, expert_up_weight, expert_down_weight)
    return layer_norm(normed.astype(jnp.float32) + expert_mix, layer_norm_gains[1], layer_norm_shifts[1]).astype(jnp.bfloat16)
```

```python
import functools

import jax
import jax.numpy as jnp
from jax import lax
from jax.experimental import pallas as pl
from jax.experimental.pallas import tpu as pltpu
from jax.sharding import PartitionSpec as P

eps_rms = 1e-06
eps_layer = 1e-05
decay_norm = 16.0
CHUNKS = 2

f32 = jnp.float32
bf16 = jnp.bfloat16
HIGHEST = lax.Precision.HIGHEST
NT = (((1,), (1,)), ((), ()))
TN = (((0,), (0,)), ((), ()))


def iota(shape, dim):
    return lax.broadcasted_iota(jnp.int32, shape, dim)


def dot(a, b, dims=(((1,), (0,)), ((), ())), precision=None):
    return lax.dot_general(a, b, dims, precision=precision, preferred_element_type=f32)


def state_kernel(key_ref, value_ref, gate_ref, offset_ref, spikes_ref, docs_ref, pack_ref, total_ref, doc_ref):
    span, channels = key_ref.shape
    heads = spikes_ref.shape[0]
    key_dim = channels // heads
    value_dim = value_ref.shape[1] // heads
    logit = gate_ref[...].astype(f32) + offset_ref[...]
    rate = (jnp.minimum(logit, 0.0) - jnp.log1p(jnp.exp(-jnp.abs(logit)))) / decay_norm
    spread = (iota((heads, channels), 1) // key_dim == iota((heads, channels), 0)).astype(f32)
    rate = rate + dot(spikes_ref[...], spread, TN, HIGHEST)
    lower = (iota((span, span), 0) >= iota((span, span), 1)).astype(f32)
    total = dot(lower, rate, precision=HIGHEST)
    total_ref[...] = total
    eye = (iota((span, span), 0) == iota((span, span), 1)).astype(f32).astype(bf16)
    doc_rows = jnp.broadcast_to(docs_ref[...].astype(f32), (128, span)).astype(bf16)
    doc_cols = dot(eye, doc_rows, NT)
    doc_ref[...] = doc_cols
    first_doc = doc_cols[0:1, :]
    last_doc = doc_cols[span - 1 : span, :]
    final = total[span - 1 : span, :]
    ends = key_ref[...].astype(f32) * jnp.exp(final - total)
    ends = jnp.where(doc_cols[:, 0:1] == last_doc[:, 0:1], ends, 0.0).astype(bf16)
    products = dot(value_ref[...], ends, TN)
    lane_head = iota((value_dim, channels), 1) // key_dim
    state = jnp.zeros((value_dim, channels), f32)
    for head in range(heads):
        state = jnp.where(lane_head == head, products[head * value_dim : (head + 1) * value_dim], state)
    pack_ref[0:value_dim, :] = state.astype(bf16)
    tail = iota((16, channels), 0)
    rows = jnp.where(tail == 0, jnp.exp(final), jnp.where(tail == 1, first_doc[:, 0:1], last_doc[:, 0:1]))
    pack_ref[value_dim : value_dim + 16, :] = rows.astype(bf16)


def scores_kernel(query_ref, key_ref, value_ref, total_ref, doc_ref, docs_ref, inner_ref, *, heads):
    span, channels = key_ref.shape
    key_dim = channels // heads
    width = value_ref.shape[1]
    value_dim = width // heads
    tile = 128
    scale = key_dim**-0.5
    xor = iota((tile, tile), 0) ^ iota((tile, tile), 1)
    causal = iota((tile, tile), 0) >= iota((tile, tile), 1)
    lane_head = iota((tile, channels), 1) // key_dim
    value_head = iota((tile, width), 1) // value_dim
    tiles = span // tile

    def rows(ref, index):
        return ref[index * tile : (index + 1) * tile, :]

    def picked(array, head):
        return jnp.where(lane_head == head, array, 0.0).astype(bf16)

    for i in range(tiles):
        total = rows(total_ref, i)
        query = rows(query_ref, i).astype(f32) * scale
        key = rows(key_ref, i).astype(f32)
        levels = []
        half = tile // 2
        while half >= 1:
            if half >= 8:
                grouped = total.reshape(tile // (2 * half), 2 * half, channels)
                mark = jnp.broadcast_to(grouped[:, half - 1 : half, :], grouped.shape).reshape(tile, channels)
            else:
                grouped = total.reshape(tile // 8, 8, channels)
                sub = iota(grouped.shape, 1) // (2 * half)
                mark = jnp.broadcast_to(grouped[:, half - 1 : half, :], grouped.shape)
                for block in range(1, 8 // (2 * half)):
                    at = block * 2 * half + half - 1
                    mark = jnp.where(sub == block, grouped[:, at : at + 1, :], mark)
                mark = mark.reshape(tile, channels)
            fade = jnp.exp(-jnp.abs(total - mark))
            levels.append((2 * half, query * fade, (key * fade).astype(bf16)))
            half //= 2
        levels.append((1, query, key.astype(bf16)))
        visible = causal & (rows(doc_ref, i)[:, 0:tile] == docs_ref[:, i * tile : (i + 1) * tile].astype(f32))
        earlier = []
        for j in range(i):
            edge = total_ref[i * tile - 1 : i * tile, :]
            far_query = query * jnp.exp(total - edge)
            far_key = (rows(key_ref, j).astype(f32) * jnp.exp(edge - rows(total_ref, j))).astype(bf16)
            same = rows(doc_ref, i)[:, 0:tile] == docs_ref[:, j * tile : (j + 1) * tile].astype(f32)
            earlier.append((j, far_query, far_key, same))
        result = jnp.zeros((tile, width), f32)
        for head in range(heads):
            score = None
            for bound, level_query, level_key in levels:
                part = dot(picked(level_query, head), level_key, NT)
                score = part if score is None else jnp.where(xor < bound, part, score)
            score = jnp.where(visible, score, 0.0).astype(bf16)
            own = jnp.where(value_head == head, rows(value_ref, i).astype(f32), 0.0).astype(bf16)
            result = result + dot(score, own)
            for j, far_query, far_key, same in earlier:
                score = jnp.where(same, dot(picked(far_query, head), far_key, NT), 0.0).astype(bf16)
                own = jnp.where(value_head == head, rows(value_ref, j).astype(f32), 0.0).astype(bf16)
                result = result + dot(score, own)
        inner_ref[i * tile : (i + 1) * tile, :] = result


def mix_kernel(place_ref, query_ref, total_ref, doc_ref, inner_ref, gate_ref, weight_ref, *refs, heads, order):
    packs, (near_ref, far_ref, mixed_ref) = refs[:-3], refs[-3:]
    span, channels = query_ref.shape
    key_dim = channels // heads
    width = inner_ref.shape[1]
    value_dim = width // heads
    here = place_ref[0]
    rank = place_ref[1]
    state = jnp.zeros((value_dim, channels), f32)
    last = jnp.full((1, channels), -1.0, f32)
    for distance in range(len(packs), 0, -1):
        pack = packs[distance - 1]
        part = pack[0:value_dim, :].astype(f32)
        extra = pack[value_dim : value_dim + 16, :].astype(f32)
        fade, first, final = extra[0:1, :], extra[1:2, :], extra[2:3, :]
        joined = ((first == final) & ((last == first) | (last < 0.0))).astype(f32)
        reached = distance <= here
        state = jnp.where(reached, state * (fade * joined) + part, state)
        last = jnp.where(reached, final, last)
    lane_head = iota((value_dim, channels), 1) // key_dim
    blocks = [jnp.where(lane_head == head, state, 0.0).astype(bf16) for head in range(heads)]
    carried = jnp.concatenate(blocks, axis=0)
    seen = query_ref[...].astype(f32) * key_dim**-0.5 * jnp.exp(total_ref[...])
    seen = jnp.where(doc_ref[:, 0:1] == last[:, 0:1], seen, 0.0).astype(bf16)
    recurrent = inner_ref[...] + dot(seen, carried, NT)
    same = (iota((width, width), 0) // value_dim == iota((width, width), 1) // value_dim).astype(f32).astype(bf16)
    square = recurrent * recurrent
    high = square.astype(bf16)
    low = (square - high.astype(f32)).astype(bf16)
    mean = (dot(high, same) + dot(low, same)) / value_dim
    gate = gate_ref[...].astype(f32)
    mixed_ref[...] = (recurrent * lax.rsqrt(mean + eps_rms) * (gate / (1.0 + jnp.exp(-gate)))).astype(bf16)
    block = span // len(order)
    half = len(order) // 2
    for number, relative in enumerate(order):
        start = pl.multiple_of((rank ^ relative) * block, block)
        out = dot(mixed_ref[pl.ds(start, block), :], weight_ref[...]).astype(bf16)
        target = near_ref if number < half else far_ref
        at = (number % half) * block
        target[at : at + block, :] = out


def normed_rows(stream, gain_row, shift_row):
    center = jnp.mean(stream, axis=-1, keepdims=True)
    moved = stream - center
    spread = jnp.mean(moved * moved, axis=-1, keepdims=True)
    return moved * lax.rsqrt(spread + eps_layer) * gain_row + shift_row


def enter_kernel(residual_ref, first_ref, second_ref, gains_ref, shifts_ref, pick_ref, normed_ref, *out_refs):
    stream = residual_ref[...].astype(f32) + first_ref[...].astype(f32) + second_ref[...].astype(f32)
    normed = normed_rows(stream, gains_ref[0:1, :], shifts_ref[0:1, :]).astype(bf16)
    normed_ref[...] = normed
    rows = out_refs[0].shape[0]
    for number, out_ref in enumerate(out_refs):
        out_ref[...] = dot(pick_ref[number * rows : (number + 1) * rows, :], normed).astype(bf16)


def leave_kernel(normed_ref, high_ref, low_ref, gains_ref, shifts_ref, *refs):
    out_ref = refs[-1]
    stream = normed_ref[...].astype(f32)
    start = 0
    for ref in refs[:-1]:
        rows = ref.shape[0]
        piece = ref[...]
        stream = stream + dot(high_ref[:, start : start + rows], piece) + dot(low_ref[:, start : start + rows], piece)
        start += rows
    out_ref[...] = normed_rows(stream, gains_ref[1:2, :], shifts_ref[1:2, :]).astype(bf16)


def call(body, outs, *args, scalars=0, scratch=()):
    vmem = pl.BlockSpec(memory_space=pltpu.VMEM)
    smem = pl.BlockSpec(memory_space=pltpu.SMEM)
    specs = [smem if n < scalars else vmem for n in range(len(args))]
    return pl.pallas_call(
        body,
        out_shape=outs,
        in_specs=specs,
        out_specs=jax.tree.map(lambda _: vmem, outs),
        scratch_shapes=scratch,
    )(*args)


def swap(array, axis, relative):
    peers = lax.axis_size(axis)
    return lax.ppermute(array, axis, [(k, k ^ relative) for k in range(peers)])


def exchange(pieces, axis):
    return [piece if d == 0 else swap(piece, axis, d) for d, piece in enumerate(pieces)]


def bits_of(peers):
    bits = []
    while peers > 1:
        peers //= 2
        bits.append(peers)
    return bits


def spread_rows(piece, axis):
    held = {0: piece}
    for bit in bits_of(lax.axis_size(axis)):
        for relative in list(held):
            held[relative ^ bit] = swap(held[relative], axis, bit)
    return held


def sum_rows(held, axis):
    for bit in reversed(bits_of(lax.axis_size(axis))):
        keep = [relative for relative in held if not relative & bit]
        got = {relative: swap(held[relative ^ bit], axis, bit) for relative in keep}
        held = {r: (held[r].astype(f32) + got[r].astype(f32)).astype(bf16) for r in keep}
    return held[0]


def on_device(
    residual,
    queries,
    projected_keys,
    values,
    projected_output_gate,
    decay_gate_input,
    decay_gate_offset,
    decay_spikes,
    documents,
    attention_output_weight,
    layer_norm_gains,
    layer_norm_shifts,
    routes,
    chosen_expert_weights,
    expert_gate_weight,
    expert_up_weight,
    expert_down_weight,
):
    span, heads = decay_spikes.shape
    channels = queries.shape[1]
    width = values.shape[1]
    value_dim = width // heads
    rows_dev, model_width = residual.shape
    groups = lax.axis_size("sp")
    parts = lax.axis_size("tp")
    here, rank = lax.axis_index("sp"), lax.axis_index("tp")
    capacity = max(2, 4 * rows_dev // groups)
    shape = jax.ShapeDtypeStruct

    docs_row = documents.reshape(1, span)
    pack, total, doc_cols = call(
        state_kernel,
        (shape((value_dim + 16, channels), bf16), shape((span, channels), f32), shape((span, 128), f32)),
        projected_keys,
        values,
        decay_gate_input,
        decay_gate_offset.reshape(1, channels),
        decay_spikes.T,
        docs_row,
    )
    packs = [
        lax.ppermute(pack, "sp", [(k, k + d) for k in range(groups - d)]) for d in range(1, groups)
    ]
    inner = call(
        functools.partial(scores_kernel, heads=heads),
        shape((span, width), f32),
        queries,
        projected_keys,
        values,
        total,
        doc_cols,
        docs_row,
    )
    order = [r for r in range(parts) if not r & 1] + [r for r in range(parts) if r & 1]
    near, far = call(
        functools.partial(mix_kernel, heads=heads, order=order),
        (shape((span // 2, model_width), bf16),) * 2,
        jnp.stack([here, rank]).astype(jnp.int32),
        queries,
        total,
        doc_cols,
        inner,
        projected_output_gate,
        attention_output_weight,
        *packs,
        scalars=1,
        scratch=(pltpu.VMEM((span, width), bf16),),
    )
    got = swap(far, "tp", 1)
    paired = (near.astype(f32) + got.astype(f32)).astype(bf16)
    held = {r: paired[(r // 2) * rows_dev : (r // 2 + 1) * rows_dev] for r in range(0, parts, 2)}
    for bit in reversed(bits_of(parts)[1:-1]):
        keep = [r for r in held if not r & bit]
        arrived = {r: swap(held[r ^ bit], "tp", bit) for r in keep}
        held = {r: (held[r].astype(f32) + arrived[r].astype(f32)).astype(bf16) for r in keep}
    top_bit = bits_of(parts)[0]
    arrived = swap(held[top_bit], "tp", top_bit)

    own_routes = lax.dynamic_slice_in_dim(routes, rank * rows_dev, rows_dev, 0)
    own_weights = lax.dynamic_slice_in_dim(chosen_expert_weights, rank * rows_dev, rows_dev, 0)
    experts = lax.broadcasted_iota(jnp.int32, (1, groups), 1) ^ here
    marks = [own_routes[:, j : j + 1] == experts for j in range(own_routes.shape[1])]
    named = functools.reduce(jnp.logical_or, marks)
    share = sum(jnp.where(mark, own_weights[:, j : j + 1], 0.0) for j, mark in enumerate(marks))
    lower = (iota((rows_dev, rows_dev), 0) > iota((rows_dev, rows_dev), 1)).astype(bf16)
    before = dot(lower, named.astype(bf16))
    place = jnp.where(named, before, -1.0)
    chunks = CHUNKS if capacity % CHUNKS == 0 else 1
    size = capacity // chunks
    seats = iota((chunks, 1, size), 0) * size + iota((chunks, 1, size), 2)
    hits = place[None, :, :, None] == seats[:, None, :, :].astype(f32).reshape(chunks, 1, 1, size)
    hits = hits.transpose(1, 0, 2, 3)
    loads = jnp.where(hits, share[:, None, :, None], 0.0).reshape(rows_dev, groups * capacity)
    high = loads.astype(bf16)
    low = (loads - high.astype(f32)).astype(bf16)
    pick = hits.reshape(rows_dev, groups * capacity).astype(bf16).T

    normed, *outgoing = call(
        enter_kernel,
        (shape((rows_dev, model_width), bf16),)
        + (shape((groups * size, model_width), bf16),) * chunks,
        residual,
        held[0],
        arrived,
        layer_norm_gains,
        layer_norm_shifts,
        pick,
    )

    gate_weight, up_weight, down_weight = expert_gate_weight[0], expert_up_weight[0], expert_down_weight[0]
    returned = []
    for out in outgoing:
        pieces = exchange([out[d * size : (d + 1) * size] for d in range(groups)], "sp")
        held = spread_rows(jnp.concatenate(pieces, axis=0), "tp")
        names = sorted(held)
        rows = jnp.concatenate([held[r] for r in names], axis=0)
        gate_val = jnp.dot(rows, gate_weight, preferred_element_type=f32)
        up_val = jnp.dot(rows, up_weight, preferred_element_type=f32)
        hidden = (jax.nn.silu(gate_val) * up_val).astype(bf16)
        result = jnp.dot(hidden, down_weight, preferred_element_type=f32).astype(bf16)
        count = groups * size
        summed = sum_rows({r: result[n * count : (n + 1) * count] for n, r in enumerate(names)}, "tp")
        returned += exchange([summed[d * size : (d + 1) * size] for d in range(groups)], "sp")
    returned = [jnp.concatenate(returned[c * groups : (c + 1) * groups], axis=0) for c in range(chunks)]
    return call(
        leave_kernel,
        shape((rows_dev, model_width), bf16),
        normed,
        high,
        low,
        layer_norm_gains,
        layer_norm_shifts,
        *returned,
    )


def solution(mesh):
    placed = (
        P(("sp", "tp"), None),
        P("sp", "tp"),
        P("sp", "tp"),
        P("sp", "tp"),
        P("sp", "tp"),
        P("sp", "tp"),
        P("tp"),
        P("sp", "tp"),
        P("sp"),
        P("tp", None),
        P(),
        P(),
        P("sp", None),
        P("sp", None),
        P("sp", None, "tp"),
        P("sp", None, "tp"),
        P("sp", "tp", None),
    )
    return jax.shard_map(
        on_device, mesh=mesh, in_specs=placed, out_specs=P(("sp", "tp"), None), check_vma=False
    )
```

```python
import functools

import jax
import jax.numpy as jnp
from jax import lax
from jax.experimental import pallas as pl
from jax.experimental.pallas import tpu as pltpu
from jax.sharding import PartitionSpec as P

eps_rms = 1e-06
eps_layer = 1e-05
decay_norm = 16.0
CHUNKS = 2

f32 = jnp.float32
bf16 = jnp.bfloat16
HIGHEST = lax.Precision.HIGHEST
NT = (((1,), (1,)), ((), ()))
TN = (((0,), (0,)), ((), ()))


def iota(shape, dim):
    return lax.broadcasted_iota(jnp.int32, shape, dim)


def dot(a, b, dims=(((1,), (0,)), ((), ())), precision=None):
    return lax.dot_general(a, b, dims, precision=precision, preferred_element_type=f32)


def state_kernel(key_ref, value_ref, gate_ref, offset_ref, spikes_ref, docs_ref, pack_ref, total_ref, doc_ref):
    span, channels = key_ref.shape
    heads = spikes_ref.shape[0]
    key_dim = channels // heads
    value_dim = value_ref.shape[1] // heads
    logit = gate_ref[...].astype(f32) + offset_ref[...]
    rate = (jnp.minimum(logit, 0.0) - jnp.log1p(jnp.exp(-jnp.abs(logit)))) / decay_norm
    spread = (iota((heads, channels), 1) // key_dim == iota((heads, channels), 0)).astype(f32)
    rate = rate + dot(spikes_ref[...], spread, TN, HIGHEST)
    lower = (iota((span, span), 0) >= iota((span, span), 1)).astype(f32)
    total = dot(lower, rate, precision=HIGHEST)
    total_ref[...] = total
    eye = (iota((span, span), 0) == iota((span, span), 1)).astype(f32).astype(bf16)
    doc_rows = jnp.broadcast_to(docs_ref[...].astype(f32), (128, span)).astype(bf16)
    doc_cols = dot(eye, doc_rows, NT)
    doc_ref[...] = doc_cols
    first_doc = doc_cols[0:1, :]
    last_doc = doc_cols[span - 1 : span, :]
    final = total[span - 1 : span, :]
    ends = key_ref[...].astype(f32) * jnp.exp(final - total)
    ends = jnp.where(doc_cols[:, 0:1] == last_doc[:, 0:1], ends, 0.0).astype(bf16)
    products = dot(value_ref[...], ends, TN)
    lane_head = iota((value_dim, channels), 1) // key_dim
    state = jnp.zeros((value_dim, channels), f32)
    for head in range(heads):
        state = jnp.where(lane_head == head, products[head * value_dim : (head + 1) * value_dim], state)
    pack_ref[0:value_dim, :] = state.astype(bf16)
    tail = iota((16, channels), 0)
    rows = jnp.where(tail == 0, jnp.exp(final), jnp.where(tail == 1, first_doc[:, 0:1], last_doc[:, 0:1]))
    pack_ref[value_dim : value_dim + 16, :] = rows.astype(bf16)


def scores_kernel(query_ref, key_ref, value_ref, total_ref, doc_ref, docs_ref, inner_ref, *, heads):
    span, channels = key_ref.shape
    key_dim = channels // heads
    width = value_ref.shape[1]
    value_dim = width // heads
    tile = 128
    scale = key_dim**-0.5
    xor = iota((tile, tile), 0) ^ iota((tile, tile), 1)
    causal = iota((tile, tile), 0) >= iota((tile, tile), 1)
    lane_head = iota((tile, channels), 1) // key_dim
    value_head = iota((tile, width), 1) // value_dim
    tiles = span // tile

    def rows(ref, index):
        return ref[index * tile : (index + 1) * tile, :]

    def picked(array, head):
        return jnp.where(lane_head == head, array, 0.0).astype(bf16)

    for i in range(tiles):
        total = rows(total_ref, i)
        query = rows(query_ref, i).astype(f32) * scale
        key = rows(key_ref, i).astype(f32)
        levels = []
        half = tile // 2
        while half >= 1:
            if half >= 8:
                grouped = total.reshape(tile // (2 * half), 2 * half, channels)
                mark = jnp.broadcast_to(grouped[:, half - 1 : half, :], grouped.shape).reshape(tile, channels)
            else:
                grouped = total.reshape(tile // 8, 8, channels)
                sub = iota(grouped.shape, 1) // (2 * half)
                mark = jnp.broadcast_to(grouped[:, half - 1 : half, :], grouped.shape)
                for block in range(1, 8 // (2 * half)):
                    at = block * 2 * half + half - 1
                    mark = jnp.where(sub == block, grouped[:, at : at + 1, :], mark)
                mark = mark.reshape(tile, channels)
            fade = jnp.exp(-jnp.abs(total - mark))
            levels.append((2 * half, query * fade, (key * fade).astype(bf16)))
            half //= 2
        levels.append((1, query, key.astype(bf16)))
        visible = causal & (rows(doc_ref, i)[:, 0:tile] == docs_ref[:, i * tile : (i + 1) * tile].astype(f32))
        earlier = []
        for j in range(i):
            edge = total_ref[i * tile - 1 : i * tile, :]
            far_query = query * jnp.exp(total - edge)
            far_key = (rows(key_ref, j).astype(f32) * jnp.exp(edge - rows(total_ref, j))).astype(bf16)
            same = rows(doc_ref, i)[:, 0:tile] == docs_ref[:, j * tile : (j + 1) * tile].astype(f32)
            earlier.append((j, far_query, far_key, same))
        result = jnp.zeros((tile, width), f32)
        for head in range(heads):
            score = None
            for bound, level_query, level_key in levels:
                part = dot(picked(level_query, head), level_key, NT)
                score = part if score is None else jnp.where(xor < bound, part, score)
            score = jnp.where(visible, score, 0.0).astype(bf16)
            own = jnp.where(value_head == head, rows(value_ref, i).astype(f32), 0.0).astype(bf16)
            result = result + dot(score, own)
            for j, far_query, far_key, same in earlier:
                score = jnp.where(same, dot(picked(far_query, head), far_key, NT), 0.0).astype(bf16)
                own = jnp.where(value_head == head, rows(value_ref, j).astype(f32), 0.0).astype(bf16)
                result = result + dot(score, own)
        inner_ref[i * tile : (i + 1) * tile, :] = result


def mix_kernel(
    place_ref, query_ref, total_ref, doc_ref, inner_ref, gate_ref, weight_ref, packs_ref, near_ref, far_ref, mixed_ref,
    *, heads, order
):
    span, channels = query_ref.shape
    key_dim = channels // heads
    width = inner_ref.shape[1]
    value_dim = width // heads
    here = place_ref[0]
    rank = place_ref[1]

    def link(k, carry):
        state, last = carry
        pack = packs_ref[here ^ k]
        part = pack[0:value_dim, :].astype(f32)
        extra = pack[value_dim : value_dim + 16, :].astype(f32)
        fade, first, final = extra[0:1, :], extra[1:2, :], extra[2:3, :]
        joined = jnp.where(first == final, 1.0, 0.0) * jnp.where((last == first) | (last < 0.0), 1.0, 0.0)
        return state * (fade * joined) + part, final

    start = (jnp.zeros((value_dim, channels), f32), jnp.full((1, channels), -1.0, f32))
    state, last = lax.fori_loop(0, here, link, start)
    lane_head = iota((value_dim, channels), 1) // key_dim
    blocks = [jnp.where(lane_head == head, state, 0.0).astype(bf16) for head in range(heads)]
    carried = jnp.concatenate(blocks, axis=0)
    seen = query_ref[...].astype(f32) * key_dim**-0.5 * jnp.exp(total_ref[...])
    seen = jnp.where(doc_ref[:, 0:1] == last[:, 0:1], seen, 0.0).astype(bf16)
    recurrent = inner_ref[...] + dot(seen, carried, NT)
    same = (iota((width, width), 0) // value_dim == iota((width, width), 1) // value_dim).astype(f32).astype(bf16)
    square = recurrent * recurrent
    high = square.astype(bf16)
    low = (square - high.astype(f32)).astype(bf16)
    mean = (dot(high, same) + dot(low, same)) / value_dim
    gate = gate_ref[...].astype(f32)
    mixed_ref[...] = (recurrent * lax.rsqrt(mean + eps_rms) * (gate / (1.0 + jnp.exp(-gate)))).astype(bf16)
    block = span // len(order)
    half = len(order) // 2
    for number, relative in enumerate(order):
        start = pl.multiple_of((rank ^ relative) * block, block)
        out = dot(mixed_ref[pl.ds(start, block), :], weight_ref[...]).astype(bf16)
        target = near_ref if number < half else far_ref
        at = (number % half) * block
        target[at : at + block, :] = out


def normed_rows(stream, gain_row, shift_row):
    center = jnp.mean(stream, axis=-1, keepdims=True)
    moved = stream - center
    spread = jnp.mean(moved * moved, axis=-1, keepdims=True)
    return moved * lax.rsqrt(spread + eps_layer) * gain_row + shift_row


def enter_kernel(residual_ref, first_ref, second_ref, gains_ref, shifts_ref, pick_ref, normed_ref, *out_refs):
    stream = residual_ref[...].astype(f32) + first_ref[...].astype(f32) + second_ref[...].astype(f32)
    normed = normed_rows(stream, gains_ref[0:1, :], shifts_ref[0:1, :]).astype(bf16)
    normed_ref[...] = normed
    rows = out_refs[0].shape[0]
    for number, out_ref in enumerate(out_refs):
        out_ref[...] = dot(pick_ref[number * rows : (number + 1) * rows, :], normed).astype(bf16)


def join_kernel(*refs):
    out_ref = refs[-1]
    rows = refs[0].shape[0]
    for number, ref in enumerate(refs[:-1]):
        out_ref[number * rows : (number + 1) * rows, :] = ref[...]


def leave_kernel(normed_ref, high_ref, low_ref, gains_ref, shifts_ref, *refs):
    out_ref, rows_ref = refs[-2:]
    join_kernel(*refs[:-2], rows_ref)
    stream = normed_ref[...].astype(f32) + dot(high_ref[...], rows_ref[...]) + dot(low_ref[...], rows_ref[...])
    out_ref[...] = normed_rows(stream, gains_ref[1:2, :], shifts_ref[1:2, :]).astype(bf16)


def expert_kernel(*refs, pieces):
    ins, (gate_hbm, up_hbm, down_hbm) = refs[:pieces], refs[pieces : pieces + 3]
    outs = refs[pieces + 3 : 2 * pieces + 3]
    gate_ref, up_ref, down_ref, rows_ref, hidden_ref, gate_sem, up_sem, down_sem = refs[2 * pieces + 3 :]
    units, model_width = down_ref.shape
    starts = list(range(0, units, 256))
    waits = []
    for number, start in enumerate(starts):
        cols = pl.ds(start, min(256, units - start))
        gate_copy = pltpu.make_async_copy(gate_hbm.at[:, cols], gate_ref.at[:, cols], gate_sem.at[number])
        up_copy = pltpu.make_async_copy(up_hbm.at[:, cols], up_ref.at[:, cols], up_sem.at[number])
        gate_copy.start()
        up_copy.start()
        waits.append((cols, gate_copy, up_copy))
    down_copy = pltpu.make_async_copy(down_hbm, down_ref, down_sem)
    down_copy.start()
    join_kernel(*ins, rows_ref)
    for cols, gate_copy, up_copy in waits:
        gate_copy.wait()
        up_copy.wait()
        gate = dot(rows_ref[...], gate_ref[:, cols])
        up = dot(rows_ref[...], up_ref[:, cols])
        hidden_ref[:, cols] = (gate / (1.0 + jnp.exp(-gate)) * up).astype(bf16)
    down_copy.wait()
    rows = outs[0].shape[0]
    step = min(512, model_width)
    for start in range(0, model_width, step):
        part = dot(hidden_ref[...], down_ref[:, start : start + step]).astype(bf16)
        for number, out_ref in enumerate(outs):
            out_ref[:, start : start + step] = part[number * rows : (number + 1) * rows]


def call(body, outs, *args, scalars=0, scratch=(), remote=(), flops=0):
    vmem = pl.BlockSpec(memory_space=pltpu.VMEM)
    smem = pl.BlockSpec(memory_space=pltpu.SMEM)
    specs = [smem if n < scalars else vmem for n in range(len(args))]
    specs += [pl.BlockSpec(memory_space=pl.ANY)] * len(remote)
    cost = pl.CostEstimate(flops=flops, transcendentals=0, bytes_accessed=flops // 100) if flops else None
    return pl.pallas_call(
        body,
        out_shape=outs,
        in_specs=specs,
        out_specs=jax.tree.map(lambda _: vmem, outs),
        scratch_shapes=scratch,
        cost_estimate=cost,
    )(*args, *remote)


def swap(array, axis, relative):
    peers = lax.axis_size(axis)
    return lax.ppermute(array, axis, [(k, k ^ relative) for k in range(peers)])


def exchange(pieces, axis):
    return [piece if d == 0 else swap(piece, axis, d) for d, piece in enumerate(pieces)]


def bits_of(peers):
    bits = []
    while peers > 1:
        peers //= 2
        bits.append(peers)
    return bits


def spread_rows(piece, axis):
    held = {0: piece}
    for bit in bits_of(lax.axis_size(axis)):
        for relative in list(held):
            held[relative ^ bit] = swap(held[relative], axis, bit)
    return held


def sum_pairs(held, axis, bit):
    keep = [relative for relative in held if not relative & bit]
    got = {relative: swap(held[relative ^ bit], axis, bit) for relative in keep}
    return {r: (held[r].astype(f32) + got[r].astype(f32)).astype(bf16) for r in keep}


def sum_rows(held, axis):
    for bit in reversed(bits_of(lax.axis_size(axis))[:-1]):
        held = sum_pairs(held, axis, bit)
    return held[0]


def on_device(
    residual,
    queries,
    projected_keys,
    values,
    projected_output_gate,
    decay_gate_input,
    decay_gate_offset,
    decay_spikes,
    documents,
    attention_output_weight,
    layer_norm_gains,
    layer_norm_shifts,
    routes,
    chosen_expert_weights,
    expert_gate_weight,
    expert_up_weight,
    expert_down_weight,
):
    span, heads = decay_spikes.shape
    channels = queries.shape[1]
    width = values.shape[1]
    value_dim = width // heads
    rows_dev, model_width = residual.shape
    groups = lax.axis_size("sp")
    parts = lax.axis_size("tp")
    here, rank = lax.axis_index("sp"), lax.axis_index("tp")
    capacity = max(2, 4 * rows_dev // groups)
    shape = jax.ShapeDtypeStruct

    docs_row = documents.reshape(1, span)
    pack, total, doc_cols = call(
        state_kernel,
        (shape((value_dim + 16, channels), bf16), shape((span, channels), f32), shape((span, 128), f32)),
        projected_keys,
        values,
        decay_gate_input,
        decay_gate_offset.reshape(1, channels),
        decay_spikes.T,
        docs_row,
    )
    packs = pack[None]
    for bit in reversed(bits_of(groups)):
        packs = jnp.concatenate([packs, swap(packs, "sp", bit)], axis=0)
    inner = call(
        functools.partial(scores_kernel, heads=heads),
        shape((span, width), f32),
        queries,
        projected_keys,
        values,
        total,
        doc_cols,
        docs_row,
        flops=2 * 9 * span * 128 * (channels + width) * heads,
    )
    order = [r for r in range(parts) if not r & 1] + [r for r in range(parts) if r & 1]
    near, far = call(
        functools.partial(mix_kernel, heads=heads, order=order),
        (shape((span // 2, model_width), bf16),) * 2,
        jnp.stack([here, rank]).astype(jnp.int32),
        queries,
        total,
        doc_cols,
        inner,
        projected_output_gate,
        attention_output_weight,
        packs,
        scalars=1,
        scratch=(pltpu.VMEM((span, width), bf16),),
    )
    got = swap(far, "tp", 1)
    paired = (near.astype(f32) + got.astype(f32)).astype(bf16)
    held = {r: paired[(r // 2) * rows_dev : (r // 2 + 1) * rows_dev] for r in range(0, parts, 2)}
    for bit in reversed(bits_of(parts)[1:-1]):
        keep = [r for r in held if not r & bit]
        arrived = {r: swap(held[r ^ bit], "tp", bit) for r in keep}
        held = {r: (held[r].astype(f32) + arrived[r].astype(f32)).astype(bf16) for r in keep}
    top_bit = bits_of(parts)[0]
    arrived = swap(held[top_bit], "tp", top_bit)

    own_routes = lax.dynamic_slice_in_dim(routes, rank * rows_dev, rows_dev, 0)
    own_weights = lax.dynamic_slice_in_dim(chosen_expert_weights, rank * rows_dev, rows_dev, 0)
    experts = lax.broadcasted_iota(jnp.int32, (1, groups), 1) ^ here
    marks = [own_routes[:, j : j + 1] == experts for j in range(own_routes.shape[1])]
    named = functools.reduce(jnp.logical_or, marks)
    share = sum(jnp.where(mark, own_weights[:, j : j + 1], 0.0) for j, mark in enumerate(marks))
    lower = (iota((rows_dev, rows_dev), 0) > iota((rows_dev, rows_dev), 1)).astype(bf16)
    before = dot(lower, named.astype(bf16))
    place = jnp.where(named, before, -1.0)
    chunks = CHUNKS if capacity % CHUNKS == 0 else 1
    size = capacity // chunks
    seats = iota((chunks, 1, size), 0) * size + iota((chunks, 1, size), 2)
    hits = place[None, :, :, None] == seats[:, None, :, :].astype(f32).reshape(chunks, 1, 1, size)
    hits = hits.transpose(1, 0, 2, 3)
    loads = jnp.where(hits, share[:, None, :, None], 0.0).reshape(rows_dev, groups * capacity)
    high = loads.astype(bf16)
    low = (loads - high.astype(f32)).astype(bf16)
    pick = hits.reshape(rows_dev, groups * capacity).astype(bf16).T

    normed, *outgoing = call(
        enter_kernel,
        (shape((rows_dev, model_width), bf16),)
        + (shape((groups * size, model_width), bf16),) * chunks,
        residual,
        held[0],
        arrived,
        layer_norm_gains,
        layer_norm_shifts,
        pick,
    )

    units = expert_gate_weight.shape[2]
    weights = (
        expert_gate_weight.reshape(model_width, units),
        expert_up_weight.reshape(model_width, units),
        expert_down_weight.reshape(units, model_width),
    )
    count = groups * size
    tiles = -(-units // 256)
    aligned = size % 16 == 0
    joined = (shape((count, model_width), bf16),)

    def joining(pieces):
        return call(join_kernel, joined, *pieces)[0] if aligned else jnp.concatenate(pieces, axis=0)

    def cut(array):
        return [array[d * size : (d + 1) * size] for d in range(groups)]

    arrived_rows = []
    for out in outgoing:
        if arrived_rows:
            arrived_rows[-1], out = lax.optimization_barrier((arrived_rows[-1], out))
        arrived_rows.append(joining(exchange(cut(out), "sp")))
    spread = [spread_rows(piece, "tp") for piece in arrived_rows]

    names = list(range(parts))
    returned, paired = [], None
    for held in spread:
        pieces = [held[r] for r in names]
        if paired is not None:
            paired, pieces = lax.optimization_barrier((paired, pieces))
            returned.append(paired)
        results = call(
            functools.partial(expert_kernel, pieces=parts),
            joined * parts,
            *pieces,
            remote=weights,
            scratch=(
                pltpu.VMEM((model_width, units), bf16),
                pltpu.VMEM((model_width, units), bf16),
                pltpu.VMEM((units, model_width), bf16),
                pltpu.VMEM((parts * count, model_width), bf16),
                pltpu.VMEM((parts * count, units), bf16),
                pltpu.SemaphoreType.DMA((tiles,)),
                pltpu.SemaphoreType.DMA((tiles,)),
                pltpu.SemaphoreType.DMA,
            ),
            flops=6 * parts * count * model_width * units,
        )
        paired = sum_pairs(dict(zip(names, results)), "tp", 1)
    returned.append(paired)
    pieces = []
    for paired in returned:
        back = exchange(cut(sum_rows(paired, "tp")), "sp")
        pieces += back if aligned else [jnp.concatenate(back, axis=0)]
    return call(
        leave_kernel,
        shape((rows_dev, model_width), bf16),
        normed,
        high,
        low,
        layer_norm_gains,
        layer_norm_shifts,
        *pieces,
        scratch=(pltpu.VMEM((chunks * count, model_width), bf16),),
    )


def solution(mesh):
    placed = (
        P(("sp", "tp"), None),
        P("sp", "tp"),
        P("sp", "tp"),
        P("sp", "tp"),
        P("sp", "tp"),
        P("sp", "tp"),
        P("tp"),
        P("sp", "tp"),
        P("sp"),
        P("tp", None),
        P(),
        P(),
        P("sp", None),
        P("sp", None),
        P("sp", None, "tp"),
        P("sp", None, "tp"),
        P("sp", "tp", None),
    )
    return jax.shard_map(
        on_device, mesh=mesh, in_specs=placed, out_specs=P(("sp", "tp"), None), check_vma=False
    )
```
